32 devices in a mesh: fs: 8 (over z, y), tp: 4 (over x, core).
Axes of the slice: x: 2, y: 2, z: 4, core: 2. Of those that a mesh axis runs over, the one named last changes fastest.
Arguments:
- model_input: bfloat16 [16384, 2048], P('fs'), may hold values from -6 to 6
- value_cotan: bfloat16 [16384, 2048], P('fs', 'tp'), may hold values from -0.046875 to 0.046875
- mixer_cotan: bfloat16 [16384, 2048], P('fs'), may hold values from -0.046875 to 0.046875
- head_output: bfloat16 [16384, 2048], P('fs', 'tp'), may hold values from -6 to 6
- value_weight: float32 [2048, 2048], P('fs', 'tp'), may hold values from -0.125 to 0.125
- value_factor: bfloat16 [2048, 512], P('fs'), may hold values from -0.125 to 0.125
- value_first: float32 [512, 2048], P('fs', 'tp'), may hold values from -3 to 3
- value_second: float32 [512, 2048], P('fs', 'tp'), may hold values from 0.02 to 0.5
- output_weight: float32 [2048, 2048], P('fs', 'tp'), may hold values from -0.125 to 0.125
- output_factor: bfloat16 [2048, 512], P('fs'), may hold values from -0.125 to 0.125
- output_first: float32 [512, 2048], P('fs', 'tp'), may hold values from -3 to 3
- output_second: float32 [512, 2048], P('fs', 'tp'), may hold values from 0.02 to 0.5
Outputs:
- value_step: float32 [2048, 2048], P('fs', 'tp')
- value_updated: float32 [2048, 2048], P('fs', 'tp')
- value_first_new: float32 [512, 2048], P('fs', 'tp')
- value_second_new: float32 [512, 2048], P('fs', 'tp')
- value_copy: bfloat16 [2048, 2048], P(None, 'tp')
- output_step: float32 [2048, 2048], P('fs', 'tp')
- output_updated: float32 [2048, 2048], P('fs', 'tp')
- output_first_new: float32 [512, 2048], P('fs', 'tp')
- output_second_new: float32 [512, 2048], P('fs', 'tp')
- output_copy: bfloat16 [2048, 2048], P(None, 'tp')
The draws below stay inside these ranges and needn't reach their ends.
All inputs are finite; a program needn't handle non-finite values.
Results may differ from the reference program's by a relative error of at most 0.0059.
Values may be sent and summed in bfloat16 or wider, within the bound.
A program may use at most 128 MiB of HBM per device.

```python
import math
import jax
import jax.numpy as jnp
from jax import lax

D = 2048
RANK = 512
TOK_DEV = 2048
HV = 2048
TOKENS = 16384
N_FS = 8


def with_spikes(array, stream_key, source, target, blocks, factor):
    def block_of(dim):
        return (jnp.arange(array.shape[dim]) // (array.shape[dim] // blocks)).reshape((-1,) + (1,) * (array.ndim - 1 - dim))

    near = jax.random.permutation(stream_key, blocks)[block_of(target)]
    second = (block_of(target) + blocks // 2) % blocks
    return jnp.where((block_of(source) == near) | (block_of(source) == second), factor * array, array)


def steps_of(stream_key, extent, shards, low, high):
    level, own = 1.0, jax.random.fold_in(stream_key, 6)
    for position, shards_of in shards:
        steps = jnp.exp(jax.random.uniform(jax.random.fold_in(own, position), (shards_of,), jnp.float32, low / len(shards), high / len(shards)))
        level = level * jnp.repeat(steps, extent[position] // shards_of).reshape([-1 if axis == position else 1 for axis in range(len(extent))])
    return level


def bell_draw(own_key, extent, spread, limit, shards=(), dtype=jnp.bfloat16):
    array = jax.random.normal(own_key, extent, jnp.float32) * spread
    if len(shards) > 0:
        array = steps_of(own_key, extent, shards, -0.22, 0.18) * array
    return jnp.clip(array, min=-limit, max=limit).astype(dtype)


def noise_with(own_key, extent, spread, bound, cuts, heavy, kind=jnp.bfloat16):
    result = spread * jax.random.normal(own_key, extent, jnp.float32)
    if cuts:
        result = result * steps_of(own_key, extent, cuts, -0.22, 0.18)
    return jnp.clip(with_spikes(result, jax.random.fold_in(own_key, 3), *heavy), -bound, bound).astype(kind)


def setup_inputs(seed: int = 0) -> dict:
    arg_keys = jax.random.split(jax.random.key(seed), 13)
    model_input = noise_with(arg_keys[0], (TOKENS, D), 1.0, 6.0, ((0, 8),), (0, 1, 8, 2.0))
    value_cotan = bell_draw(arg_keys[1], (TOKENS, HV), ((TOK_DEV * N_FS) ** -0.5), 0.046875, ((0, 8), (1, 4)))
    mixer_cotan = noise_with(arg_keys[2], (TOKENS, D), ((TOK_DEV * N_FS) ** -0.5), 0.046875, ((0, 8),), (0, 1, 8, 2.0))
    head_output = bell_draw(arg_keys[3], (TOKENS, HV), 1.0, 6.0, ((0, 8), (1, 4)))
    value_weight = bell_draw(arg_keys[4], (D, HV), D ** -0.5, 0.125, ((0, 8), (1, 4)), jnp.float32)
    value_factor = bell_draw(arg_keys[5], (D, RANK), D ** -0.5, 0.125, ((0, 8),))
    value_first = bell_draw(arg_keys[6], (RANK, HV), 0.5, 3.0, ((0, 8), (1, 4)), jnp.float32)
    value_second = jnp.clip(jnp.exp(math.log(0.5) - 3.218876 * jax.random.uniform(arg_keys[7], (RANK, HV), jnp.float32) ** steps_of(arg_keys[7], (RANK, HV), ((0, 8), (1, 4)), -0.2, 0.2)), 0.02, 0.5)
    output_weight = bell_draw(arg_keys[8], (D, HV), HV ** -0.5, 0.125, ((0, 8), (1, 4)), jnp.float32)
    output_factor = bell_draw(arg_keys[9], (D, RANK), D ** -0.5, 0.125, ((0, 8),))
    output_first = bell_draw(arg_keys[10], (RANK, HV), 0.5, 3.0, ((0, 8), (1, 4)), jnp.float32)
    output_second = jnp.clip(jnp.exp(math.log(0.5) - 3.218876 * jax.random.uniform(arg_keys[11], (RANK, HV), jnp.float32) ** steps_of(arg_keys[11], (RANK, HV), ((0, 8), (1, 4)), -0.2, 0.2)), 0.02, 0.5)
    return dict(model_input=model_input, value_cotan=value_cotan, mixer_cotan=mixer_cotan, head_output=head_output, value_weight=value_weight, value_factor=value_factor, value_first=value_first, value_second=value_second, output_weight=output_weight, output_factor=output_factor, output_first=output_first, output_second=output_second)


beta_first = 0.8
beta_second = 0.9
step_rate = 0.02
scale_floor = 0.25
tiny_eps = 1e-08

def low_rank(rows_in, cols_in, factor, first_moment, second_moment):
    gradient = jnp.dot(rows_in.T, cols_in, preferred_element_type=jnp.float32)
    projected = jnp.dot(factor.astype(jnp.float32).T, gradient, precision=lax.Precision.HIGHEST)
    first_new = beta_first * first_moment + (1.0 - beta_first) * projected
    second_new = beta_second * second_moment + (1.0 - beta_second) * projected * projected
    direction = (first_new / (jnp.sqrt(second_new) + tiny_eps)).astype(jnp.bfloat16)
    expanded = jnp.dot(factor, direction, preferred_element_type=jnp.float32)
    return (expanded, first_new, second_new)

def finish(expanded, weight):
    mean_square = jnp.sum(expanded * expanded) / (D * HV)
    update_step = step_rate / jnp.sqrt(mean_square + scale_floor) * expanded
    updated = weight - update_step
    return (update_step, updated, updated.astype(jnp.bfloat16))

def reference(model_input, value_cotan, mixer_cotan, head_output, value_weight, value_factor, value_first, value_second, output_weight, output_factor, output_first, output_second):
    value_exp, value_fnew, value_snew = low_rank(model_input, value_cotan, value_factor, value_first, value_second)
    output_exp, output_fnew, output_snew = low_rank(mixer_cotan, head_output, output_factor, output_first, output_second)
    value_step, value_updated, value_copy = finish(value_exp, value_weight)
    output_step, output_updated, output_copy = finish(output_exp, output_weight)
    return (value_step, value_updated, value_fnew, value_snew, value_copy, output_step, output_updated, output_fnew, output_snew, output_copy)
```

```python
import functools

import jax
import jax.numpy as jnp
from jax import lax
from jax.experimental import pallas as pl
from jax.experimental.pallas import tpu as pltpu
from jax.sharding import PartitionSpec as P

beta_first = 0.8
beta_second = 0.9
step_rate = 0.02
scale_floor = 0.25
tiny_eps = 1e-08

MESH = pl.DeviceIdType.MESH
F32 = jnp.float32
BF16 = jnp.bfloat16
VMEM_LIMIT = 67_000_000
W_HOOK = (0, 1, 2)


def kernel(
    n,
    ntp,
    rows_v, cols_v, rows_o, cols_o,
    fac_ref, w_v, w_o, first_v, first_o, second_v, second_o,
    step_v, upd_v, fnew_v, snew_v, copy_v,
    step_o, upd_o, fnew_o, snew_o, copy_o,
    rows, cols, fg, wg, acc, e_buf, pf, pg, send_a, recv_a, send_b, recv_b,
    dirg, ss, ssg,
    sem_rows, sem_cols,
    fs_z, fr_z, fs_y, fr_y, fs_c, fr_c,
    ws_z, wr_z, ws_y, wr_y,
    as_, ar, bs, br,
    ds_z, dr_z, ds_y, dr_y,
    ps, pr,
):
    nz = n // 2
    me = lax.axis_index("fs")
    tp = lax.axis_index("tp")
    z, y = me // 2, lax.rem(me, 2)
    ybar = 1 - y
    mate = 2 * z + ybar
    core = lax.rem(tp, 2)
    other = 1 - core
    twin = tp + 1 - 2 * core
    T, D = rows_v.shape
    C = cols_v.shape[1]
    R, K = fac_ref.shape[1:]
    k = first_v.shape[0]
    TC = 512

    def zup(d):
        return lax.rem(z + d, nz)

    def zdn(d):
        return lax.rem(z + nz - d, nz)

    def rcopy(src, dst, ssem, rsem, dev):
        return pltpu.make_async_remote_copy(
            src_ref=src, dst_ref=dst, send_sem=ssem, recv_sem=rsem,
            device_id=dev, device_id_type=MESH,
        )

    def fsdev(i):
        return (i, tp)

    loads = []
    for m, (r, c) in enumerate(((rows_v, cols_v), (rows_o, cols_o))):
        loads.append(pltpu.make_async_copy(r, rows.at[m], sem_rows.at[m]))
        loads.append(pltpu.make_async_copy(c, cols.at[m], sem_cols.at[m]))
    for i in (0, 2, 1, 3):
        loads[i].start()

    barrier = pltpu.get_barrier_semaphore()
    for d in range(1, nz):
        pl.semaphore_signal(
            barrier, inc=1, device_id=fsdev(2 * zup(d) + y), device_id_type=MESH
        )
    pl.semaphore_signal(barrier, inc=1, device_id=fsdev(mate), device_id_type=MESH)
    for q in range(1, ntp):
        pl.semaphore_signal(
            barrier, inc=1, device_id=(me, lax.rem(tp + q, ntp)), device_id_type=MESH
        )
    pl.semaphore_wait(barrier, nz - 1 + 1 + ntp - 1)

    pend = []

    for d in list(range(1, nz)):
        c = rcopy(fac_ref.at[core], fg.at[core, me], fs_z.at[d], fr_z.at[d], fsdev(2 * zup(d) + y))
        c.start()
        pend.append(c)
    c = rcopy(fac_ref.at[core], fg.at[core, me], fs_y.at[0], fr_y.at[0], fsdev(mate))
    c.start()
    pend.append(c)
    for m in range(2):
        fg[m, me] = fac_ref[m]
    wg[me, 0] = w_v[...].astype(BF16)
    wg[me, 1] = w_o[...].astype(BF16)

    def w_send(d):
        if d == 0:
            c = rcopy(wg.at[me], wg.at[me], ws_y.at[0], wr_y.at[0], fsdev(mate))
        else:
            c = rcopy(wg.at[me], wg.at[me], ws_z.at[d], wr_z.at[d], fsdev(2 * zup(d) + y))
        c.start()
        pend.append(c)

    def w_forward(d):
        i = 2 * zdn(d) + y
        rcopy(wg.at[i], wg.at[i], ws_z.at[d], wr_z.at[d], fsdev(mate)).wait_recv()
        c = rcopy(wg.at[i], wg.at[i], ws_y.at[d], wr_y.at[d], fsdev(mate))
        c.start()
        pend.append(c)

    def w_finish(d):
        i = 2 * zdn(d) + ybar
        rcopy(wg.at[i], wg.at[i], ws_y.at[d], wr_y.at[d], fsdev(mate)).wait_recv()

    def to_twin(i, q):
        c = rcopy(fg.at[core, i], fg.at[core, i], fs_c.at[q], fr_c.at[q], (me, twin))
        c.start()
        pend.append(c)

    def f_recv(sems, d, i):
        rcopy(fg.at[core, i], fg.at[core, i], fs_z.at[0], sems.at[d], fsdev(mate)).wait_recv()

    def f_recv_twin(i, q):
        rcopy(fg.at[other, i], fg.at[other, i], fs_c.at[0], fr_c.at[q], (me, twin)).wait_recv()

    def accumulate(m, d):
        p = zdn(d)
        pair = jnp.concatenate([fg[m, 2 * p], fg[m, 2 * p + 1]], axis=0)
        pair_t = pair.T

        @pl.loop(0, T // TC)
        def _(t):
            at = pl.ds(pl.multiple_of(t * TC, TC), TC)
            lhs = rows[m, at, pl.ds(pl.multiple_of(p * 2 * R, 2 * R), 2 * R)]
            prod = lax.dot_general(
                pair_t, lhs, (((1,), (1,)), ((), ())), preferred_element_type=F32
            )
            if d == 0:
                acc[m, :, at] = prod
            else:
                acc[m, :, at] += prod

    for d in range(nz):
        if d > 0:
            i = 2 * zdn(d) + y
            f_recv(fr_z, d, i)
            c = rcopy(fg.at[core, i], fg.at[core, i], fs_y.at[d], fr_y.at[d], fsdev(mate))
            c.start()
            pend.append(c)
            to_twin(i, 2 * d)
        i = 2 * zdn(d) + ybar
        f_recv(fr_y, d, i)
        to_twin(i, 2 * d + 1)
        if d == 0:
            for h in range(nz):
                if h < len(W_HOOK) and W_HOOK[h] == 0 or h >= len(W_HOOK):
                    w_send(h)
            loads[0].wait()
            loads[2].wait()
        accumulate(core, d)
        if d > 0:
            f_recv_twin(2 * zdn(d) + y, 2 * d)
        f_recv_twin(i, 2 * d + 1)
        accumulate(other, d)
    loads[1].wait()
    loads[3].wait()

    def hook(v):
        for h in range(min(nz, len(W_HOOK))):
            if W_HOOK[h] == v:
                w_send(h)

    def partial_products(m):
        @pl.loop(0, T // TC)
        def _(t):
            at = pl.ds(pl.multiple_of(t * TC, TC), TC)
            red = acc[m, :, at].astype(BF16)
            prod = jnp.dot(red, cols[m, at, :], preferred_element_type=F32)
            prod = prod.reshape(n, k, C)

            @pl.when(t == 0)
            def _():
                pf[m] = prod

            @pl.when(t > 0)
            def _():
                pf[m] += prod

        for h in range(nz):
            send_a[m, h] = pf[m, 2 * zup(h) + ybar].astype(BF16)
        for h in [*range(1, nz), 0]:
            c = rcopy(
                send_a.at[m, h], recv_a.at[m, h], as_.at[m, h], ar.at[m, h], fsdev(mate)
            )
            c.start()
            pend.append(c)

    def middle(m):
        for h in [*range(1, nz), 0]:
            rcopy(
                send_a.at[m, h], recv_a.at[m, h], as_.at[m, h], ar.at[m, h], fsdev(mate)
            ).wait_recv()
            tot = pf[m, 2 * zup(h) + y] + recv_a[m, h].astype(F32)
            if h == 0:
                pg[m] = tot
            else:
                send_b[m, h] = tot.astype(BF16)
                c = rcopy(
                    send_b.at[m, h], recv_b.at[m, h], bs.at[m, h], br.at[m, h],
                    fsdev(2 * zup(h) + y),
                )
                c.start()
                pend.append(c)

    def moments(m, first, second, fnew, snew):
        tot = pg[m]
        for h in range(1, nz):
            rcopy(
                send_b.at[m, h], recv_b.at[m, h], bs.at[m, h], br.at[m, h], fsdev(mate)
            ).wait_recv()
            tot = tot + recv_b[m, h].astype(F32)
        f = beta_first * first[...] + (1.0 - beta_first) * tot
        s = beta_second * second[...] + (1.0 - beta_second) * tot * tot
        fnew[...] = f
        snew[...] = s
        dirg[m, me] = (f / (jnp.sqrt(s) + tiny_eps)).astype(BF16)
        for h in range(1, nz):
            c = rcopy(
                dirg.at[m, me], dirg.at[m, me], ds_z.at[m, h], dr_z.at[m, h],
                fsdev(2 * zup(h) + y),
            )
            c.start()
            pend.append(c)
        c = rcopy(dirg.at[m, me], dirg.at[m, me], ds_y.at[m, 0], dr_y.at[m, 0], fsdev(mate))
        c.start()
        pend.append(c)

    def dir_forward(m):
        for h in range(1, nz):
            i = 2 * zdn(h) + y
            rcopy(
                dirg.at[m, i], dirg.at[m, i], ds_z.at[m, h], dr_z.at[m, h], fsdev(mate)
            ).wait_recv()
            c = rcopy(dirg.at[m, i], dirg.at[m, i], ds_y.at[m, h], dr_y.at[m, h], fsdev(mate))
            c.start()
            pend.append(c)

    def expand(m):
        for h in range(nz):
            i = 2 * zdn(h) + ybar
            rcopy(
                dirg.at[m, i], dirg.at[m, i], ds_y.at[m, h], dr_y.at[m, h], fsdev(mate)
            ).wait_recv()
        ss[m] = jnp.zeros(ss.shape[1:], F32)

        @pl.loop(0, nz)
        def _(b):
            lhs = fg[m, pl.ds(2 * b, 2)].reshape(2 * R, K)
            ex = jnp.dot(lhs, dirg[m].reshape(n * k, C), preferred_element_type=F32)
            e_buf[m, pl.ds(2 * b, 2)] = ex.reshape(2, R, C)
            ss[m] += jnp.sum((ex * ex).reshape(2 * R // 8, 8, C), axis=0)

        for q in range(1, ntp):
            c = rcopy(
                ss.at[m], ssg.at[m, q], ps.at[m, q], pr.at[m, q],
                (me, lax.rem(tp + q, ntp)),
            )
            c.start()
            pend.append(c)

    def finish(m, weight, step, upd, copy):
        tot = ss[m]
        for q in range(1, ntp):
            rcopy(ss.at[m], ssg.at[m, q], ps.at[m, q], pr.at[m, q], (me, twin)).wait_recv()
            tot = tot + ssg[m, q]
        mean = jnp.sum(tot, keepdims=True) / (n * R * C * ntp)
        scale = step_rate / jnp.sqrt(mean + scale_floor)
        s = scale * e_buf[m, me]
        step[...] = s
        upd[...] = weight[...] - s

        @pl.loop(0, n)
        def _(b):
            at = pl.ds(pl.multiple_of(b * R, R), R)
            copy[at, :] = (wg[b, m].astype(F32) - scale * e_buf[m, b]).astype(BF16)

    partial_products(0)
    partial_products(1)
    middle(0)
    middle(1)
    hook(1)
    moments(0, first_v, second_v, fnew_v, snew_v)
    moments(1, first_o, second_o, fnew_o, snew_o)
    hook(2)
    dir_forward(0)
    dir_forward(1)
    expand(0)
    expand(1)
    for h in range(1, nz):
        w_forward(h)
    for h in range(nz):
        w_finish(h)
    finish(0, w_v, step_v, upd_v, copy_v)
    finish(1, w_o, step_o, upd_o, copy_o)
    for c in pend:
        c.wait_send()


def local(
    n, ntp,
    model_input, value_cotan, mixer_cotan, head_output,
    value_weight, value_factor, value_first, value_second,
    output_weight, output_factor, output_first, output_second,
):
    T, D = model_input.shape
    C = value_cotan.shape[1]
    R, K = value_factor.shape
    k = value_first.shape[0]
    nz = n // 2
    vm = pl.BlockSpec(memory_space=pltpu.VMEM)
    hbm = pl.BlockSpec(memory_space=pl.ANY)
    wide = jax.ShapeDtypeStruct((R, C), F32)
    mom = jax.ShapeDtypeStruct((k, C), F32)
    full = jax.ShapeDtypeStruct((n * R, C), BF16)
    dma = pltpu.SemaphoreType.DMA
    return pl.pallas_call(
        functools.partial(kernel, n, ntp),
        out_shape=(wide, wide, mom, mom, full) * 2,
        in_specs=[hbm] * 4 + [vm] * 7,
        out_specs=(vm,) * 10,
        scratch_shapes=[
            pltpu.VMEM((2, T, D), BF16),
            pltpu.VMEM((2, T, C), BF16),
            pltpu.VMEM((2, n, R, K), BF16),
            pltpu.VMEM((n, 2, R, C), BF16),
            pltpu.VMEM((2, K, T), F32),
            pltpu.VMEM((2, n, R, C), F32),
            pltpu.VMEM((2, n, k, C), F32),
            pltpu.VMEM((2, k, C), F32),
            pltpu.VMEM((2, nz, k, C), BF16),
            pltpu.VMEM((2, nz, k, C), BF16),
            pltpu.VMEM((2, nz, k, C), BF16),
            pltpu.VMEM((2, nz, k, C), BF16),
            pltpu.VMEM((2, n, k, C), BF16),
            pltpu.VMEM((2, 8, C), F32),
            pltpu.VMEM((2, ntp, 8, C), F32),
            dma((2,)), dma((2,)),
            dma((nz,)), dma((nz,)), dma((nz,)), dma((nz,)), dma((n,)), dma((n,)),
            dma((nz,)), dma((nz,)), dma((nz,)), dma((nz,)),
            dma((2, nz)), dma((2, nz)), dma((2, nz)), dma((2, nz)),
            dma((2, nz)), dma((2, nz)), dma((2, nz)), dma((2, nz)),
            dma((2, ntp)), dma((2, ntp)),
        ],
        compiler_params=pltpu.CompilerParams(
            collective_id=0, has_side_effects=True, vmem_limit_bytes=VMEM_LIMIT
        ),
    )(
        model_input, value_cotan, mixer_cotan, head_output,
        jnp.stack([value_factor, output_factor]),
        value_weight, output_weight,
        value_first, output_first, value_second, output_second,
    )


def solution(mesh):
    rows, both, full = P("fs", None), P("fs", "tp"), P(None, "tp")
    return jax.shard_map(
        functools.partial(local, mesh.shape["fs"], mesh.shape["tp"]),
        mesh=mesh,
        in_specs=(rows, both, rows, both) + (both, rows, both, both) * 2,
        out_specs=(both, both, both, both, full) * 2,
        check_vma=False,
    )
```

```python
import functools

import jax
import jax.numpy as jnp
from jax import lax
from jax.experimental import pallas as pl
from jax.experimental.pallas import tpu as pltpu
from jax.sharding import PartitionSpec as P

beta_first = 0.8
beta_second = 0.9
step_rate = 0.02
scale_floor = 0.25
tiny_eps = 1e-08

MESH = pl.DeviceIdType.MESH
F32 = jnp.float32
BF16 = jnp.bfloat16
VMEM_LIMIT = 67_000_000
PLAN = (((1, 0), (1, 1), (1, 3), (1, 2)), ((2, 3),), ((2, 2),), (), (), (), ((2, 1),))


def kernel(
    n,
    ntp,
    rows_v, cols_v, rows_o, cols_o,
    fac_ref, w_v, w_o, first_v, first_o, second_v, second_o,
    step_v, upd_v, fnew_v, snew_v, copy_v,
    step_o, upd_o, fnew_o, snew_o, copy_o,
    rows, cols, fg, wg, acc, e_buf, pf, pg, send_a, recv_a, send_b, recv_b,
    dirg, ss, ssg,
    sem_rows, sem_cols,
    fs_z, fr_z, fs_y, fr_y, fs_x, fr_x, fs_c, fr_c,
    ws_z, wr_z, ws_y, wr_y,
    as_, ar, bs, br,
    ds_z, dr_z, ds_y, dr_y,
    ps, pr,
):
    nz = n // 2
    me = lax.axis_index("fs")
    tp = lax.axis_index("tp")
    z, y = me // 2, lax.rem(me, 2)
    ybar = 1 - y
    mate = 2 * z + ybar
    core = lax.rem(tp, 2)
    other = 1 - core
    twin = tp + 1 - 2 * core
    half = tp // 2
    far = 1 - half
    across = tp + 2 - 4 * half
    T, D = rows_v.shape
    C = cols_v.shape[1]
    R, K = fac_ref.shape[2] * 2, fac_ref.shape[3]
    k = first_v.shape[0]
    TC = 512

    def zup(d):
        return lax.rem(z + d, nz)

    def zdn(d):
        return lax.rem(z + nz - d, nz)

    def rcopy(src, dst, ssem, rsem, dev):
        return pltpu.make_async_remote_copy(
            src_ref=src, dst_ref=dst, send_sem=ssem, recv_sem=rsem,
            device_id=dev, device_id_type=MESH,
        )

    def fsdev(i):
        return (i, tp)

    loads = []
    for m, (r, c) in enumerate(((rows_v, cols_v), (rows_o, cols_o))):
        loads.append(pltpu.make_async_copy(r, rows.at[m], sem_rows.at[m]))
        loads.append(pltpu.make_async_copy(c, cols.at[m], sem_cols.at[m]))
    for i in (0, 2, 1, 3):
        loads[i].start()

    barrier = pltpu.get_barrier_semaphore()
    for d in range(1, nz):
        pl.semaphore_signal(
            barrier, inc=1, device_id=fsdev(2 * zup(d) + y), device_id_type=MESH
        )
    pl.semaphore_signal(barrier, inc=1, device_id=fsdev(mate), device_id_type=MESH)
    for q in range(1, ntp):
        pl.semaphore_signal(
            barrier, inc=1, device_id=(me, lax.rem(tp + q, ntp)), device_id_type=MESH
        )
    pl.semaphore_wait(barrier, nz - 1 + 1 + ntp - 1)

    pend = []

    for d in list(range(1, nz)):
        c = rcopy(fac_ref.at[core, half], fg.at[core, me, half], fs_z.at[d], fr_z.at[d], fsdev(2 * zup(d) + y))
        c.start()
        pend.append(c)
    c = rcopy(fac_ref.at[core, half], fg.at[core, me, half], fs_y.at[0], fr_y.at[0], fsdev(mate))
    c.start()
    pend.append(c)
    for m in range(2):
        fg[m, me] = fac_ref[m]
    wg[me, 0] = w_v[...].astype(BF16)
    wg[me, 1] = w_o[...].astype(BF16)

    def w_send(d):
        if d == 0:
            c = rcopy(wg.at[me], wg.at[me], ws_y.at[0], wr_y.at[0], fsdev(mate))
        else:
            c = rcopy(wg.at[me], wg.at[me], ws_z.at[d], wr_z.at[d], fsdev(2 * zup(d) + y))
        c.start()
        pend.append(c)

    def w_forward(d):
        i = 2 * zdn(d) + y
        rcopy(wg.at[i], wg.at[i], ws_z.at[d], wr_z.at[d], fsdev(mate)).wait_recv()
        c = rcopy(wg.at[i], wg.at[i], ws_y.at[d], wr_y.at[d], fsdev(mate))
        c.start()
        pend.append(c)

    def w_finish(d):
        i = 2 * zdn(d) + ybar
        rcopy(wg.at[i], wg.at[i], ws_y.at[d], wr_y.at[d], fsdev(mate)).wait_recv()

    def act(point):
        for kind, d in PLAN[point]:
            if d < nz:
                (w_send if kind == 1 else w_forward)(d)
        for d in range(4, nz):
            if point == 0:
                w_send(d)
            if point == 5:
                w_forward(d)

    def mine(i):
        return fg.at[core, i, half]

    def to_mates(i, q):
        for src, ssem, rsem, dev in (
            (mine(i), fs_x.at[q], fr_x.at[q], (me, across)),
            (mine(i), fs_c.at[0, q], fr_c.at[0, q], (me, twin)),
        ):
            c = rcopy(src, src, ssem, rsem, dev)
            c.start()
            pend.append(c)

    def f_recv(sems, d, i):
        rcopy(mine(i), mine(i), fs_z.at[0], sems.at[d], fsdev(mate)).wait_recv()

    def f_recv_across(i, q):
        r = fg.at[core, i, far]
        rcopy(r, r, fs_x.at[q], fr_x.at[q], (me, across)).wait_recv()
        c = rcopy(r, r, fs_c.at[1, q], fr_c.at[1, q], (me, twin))
        c.start()
        pend.append(c)

    def f_recv_twin(i, q):
        for g, h in ((0, half), (1, far)):
            r = fg.at[other, i, h]
            rcopy(r, r, fs_c.at[g, q], fr_c.at[g, q], (me, twin)).wait_recv()

    def accumulate(m, d):
        p = zdn(d)
        pair_t = fg[m, pl.ds(2 * p, 2)].reshape(2 * R, K).T

        @pl.loop(0, T // TC)
        def _(t):
            at = pl.ds(pl.multiple_of(t * TC, TC), TC)
            lhs = rows[m, at, pl.ds(pl.multiple_of(p * 2 * R, 2 * R), 2 * R)]
            prod = lax.dot_general(
                pair_t, lhs, (((1,), (1,)), ((), ())), preferred_element_type=F32
            )
            if d == 0:
                acc[m, :, at] = prod
            else:
                acc[m, :, at] += prod

    def arrive(d):
        if d > 0:
            i = 2 * zdn(d) + y
            f_recv(fr_z, d, i)
            c = rcopy(mine(i), mine(i), fs_y.at[d], fr_y.at[d], fsdev(mate))
            c.start()
            pend.append(c)
            to_mates(i, 2 * d)
        i = 2 * zdn(d) + ybar
        f_recv(fr_y, d, i)
        to_mates(i, 2 * d + 1)

    def complete(d):
        qs = ([(2 * zdn(d) + y, 2 * d)] if d else []) + [(2 * zdn(d) + ybar, 2 * d + 1)]
        for i, q in qs:
            f_recv_across(i, q)
        if d == 0:
            loads[0].wait()
            loads[2].wait()
        accumulate(core, d)
        for i, q in qs:
            f_recv_twin(i, q)
        accumulate(other, d)

    for d in range(nz):
        arrive(d)
        if d == 0:
            act(0)
        else:
            complete(d - 1)
    act(6)
    complete(nz - 1)
    loads[1].wait()
    loads[3].wait()

    def partial_products(m):
        @pl.loop(0, T // TC)
        def _(t):
            at = pl.ds(pl.multiple_of(t * TC, TC), TC)
            red = acc[m, :, at].astype(BF16)
            prod = jnp.dot(red, cols[m, at, :], preferred_element_type=F32)
            prod = prod.reshape(n, k, C)

            @pl.when(t == 0)
            def _():
                pf[m] = prod

            @pl.when(t > 0)
            def _():
                pf[m] += prod

        for h in range(nz):
            send_a[m, h] = pf[m, 2 * zup(h) + ybar].astype(BF16)
        for h in [*range(1, nz), 0]:
            c = rcopy(
                send_a.at[m, h], recv_a.at[m, h], as_.at[m, h], ar.at[m, h], fsdev(mate)
            )
            c.start()
            pend.append(c)

    def middle(m):
        for h in [*range(1, nz), 0]:
            rcopy(
                send_a.at[m, h], recv_a.at[m, h], as_.at[m, h], ar.at[m, h], fsdev(mate)
            ).wait_recv()
            tot = pf[m, 2 * zup(h) + y] + recv_a[m, h].astype(F32)
            if h == 0:
                pg[m] = tot
            else:
                send_b[m, h] = tot.astype(BF16)
                c = rcopy(
                    send_b.at[m, h], recv_b.at[m, h], bs.at[m, h], br.at[m, h],
                    fsdev(2 * zup(h) + y),
                )
                c.start()
                pend.append(c)

    def moments(m, first, second, fnew, snew):
        tot = pg[m]
        for h in range(1, nz):
            rcopy(
                send_b.at[m, h], recv_b.at[m, h], bs.at[m, h], br.at[m, h], fsdev(mate)
            ).wait_recv()
            tot = tot + recv_b[m, h].astype(F32)
        f = beta_first * first[...] + (1.0 - beta_first) * tot
        s = beta_second * second[...] + (1.0 - beta_second) * tot * tot
        fnew[...] = f
        snew[...] = s
        dirg[m, me] = (f / (jnp.sqrt(s) + tiny_eps)).astype(BF16)
        for h in range(1, nz):
            c = rcopy(
                dirg.at[m, me], dirg.at[m, me], ds_z.at[m, h], dr_z.at[m, h],
                fsdev(2 * zup(h) + y),
            )
            c.start()
            pend.append(c)
        c = rcopy(dirg.at[m, me], dirg.at[m, me], ds_y.at[m, 0], dr_y.at[m, 0], fsdev(mate))
        c.start()
        pend.append(c)

    def dir_forward(m):
        for h in range(1, nz):
            i = 2 * zdn(h) + y
            rcopy(
                dirg.at[m, i], dirg.at[m, i], ds_z.at[m, h], dr_z.at[m, h], fsdev(mate)
            ).wait_recv()
            c = rcopy(dirg.at[m, i], dirg.at[m, i], ds_y.at[m, h], dr_y.at[m, h], fsdev(mate))
            c.start()
            pend.append(c)

    def expand(m):
        for h in range(nz):
            i = 2 * zdn(h) + ybar
            rcopy(
                dirg.at[m, i], dirg.at[m, i], ds_y.at[m, h], dr_y.at[m, h], fsdev(mate)
            ).wait_recv()
        ss[m] = jnp.zeros(ss.shape[1:], F32)

        @pl.loop(0, nz)
        def _(b):
            lhs = fg[m, pl.ds(2 * b, 2)].reshape(2 * R, K)
            ex = jnp.dot(lhs, dirg[m].reshape(n * k, C), preferred_element_type=F32)
            e_buf[m, pl.ds(2 * b, 2)] = ex.reshape(2, R, C)
            ss[m] += jnp.sum((ex * ex).reshape(2 * R // 8, 8, C), axis=0)

        for q in range(1, ntp):
            c = rcopy(
                ss.at[m], ssg.at[m, q], ps.at[m, q], pr.at[m, q],
                (me, lax.rem(tp + q, ntp)),
            )
            c.start()
            pend.append(c)

    def finish(m, weight, step, upd, copy):
        tot = ss[m]
        for q in range(1, ntp):
            rcopy(ss.at[m], ssg.at[m, q], ps.at[m, q], pr.at[m, q], (me, twin)).wait_recv()
            tot = tot + ssg[m, q]
        mean = jnp.sum(tot, keepdims=True) / (n * R * C * ntp)
        scale = step_rate / jnp.sqrt(mean + scale_floor)
        s = scale * e_buf[m, me]
        step[...] = s
        upd[...] = weight[...] - s

        @pl.loop(0, n)
        def _(b):
            at = pl.ds(pl.multiple_of(b * R, R), R)
            copy[at, :] = (wg[b, m].astype(F32) - scale * e_buf[m, b]).astype(BF16)

    partial_products(0)
    partial_products(1)
    act(1)
    middle(0)
    middle(1)
    act(2)
    moments(0, first_v, second_v, fnew_v, snew_v)
    moments(1, first_o, second_o, fnew_o, snew_o)
    act(3)
    dir_forward(0)
    dir_forward(1)
    act(4)
    expand(0)
    expand(1)
    act(5)
    for h in range(nz):
        w_finish(h)
    finish(0, w_v, step_v, upd_v, copy_v)
    finish(1, w_o, step_o, upd_o, copy_o)
    for c in pend:
        c.wait_send()


def local(
    n, ntp,
    model_input, value_cotan, mixer_cotan, head_output,
    value_weight, value_factor, value_first, value_second,
    output_weight, output_factor, output_first, output_second,
):
    T, D = model_input.shape
    C = value_cotan.shape[1]
    R, K = value_factor.shape
    k = value_first.shape[0]
    nz = n // 2
    vm = pl.BlockSpec(memory_space=pltpu.VMEM)
    hbm = pl.BlockSpec(memory_space=pl.ANY)
    wide = jax.ShapeDtypeStruct((R, C), F32)
    mom = jax.ShapeDtypeStruct((k, C), F32)
    full = jax.ShapeDtypeStruct((n * R, C), BF16)
    dma = pltpu.SemaphoreType.DMA
    return pl.pallas_call(
        functools.partial(kernel, n, ntp),
        out_shape=(wide, wide, mom, mom, full) * 2,
        in_specs=[hbm] * 4 + [vm] * 7,
        out_specs=(vm,) * 10,
        scratch_shapes=[
            pltpu.VMEM((2, T, D), BF16),
            pltpu.VMEM((2, T, C), BF16),
            pltpu.VMEM((2, n, 2, R // 2, K), BF16),
            pltpu.VMEM((n, 2, R, C), BF16),
            pltpu.VMEM((2, K, T), F32),
            pltpu.VMEM((2, n, R, C), F32),
            pltpu.VMEM((2, n, k, C), F32),
            pltpu.VMEM((2, k, C), F32),
            pltpu.VMEM((2, nz, k, C), BF16),
            pltpu.VMEM((2, nz, k, C), BF16),
            pltpu.VMEM((2, nz, k, C), BF16),
            pltpu.VMEM((2, nz, k, C), BF16),
            pltpu.VMEM((2, n, k, C), BF16),
            pltpu.VMEM((2, 8, C), F32),
            pltpu.VMEM((2, ntp, 8, C), F32),
            dma((2,)), dma((2,)),
            dma((nz,)), dma((nz,)), dma((nz,)), dma((nz,)), dma((n,)), dma((n,)), dma((2, n)), dma((2, n)),
            dma((nz,)), dma((nz,)), dma((nz,)), dma((nz,)),
            dma((2, nz)), dma((2, nz)), dma((2, nz)), dma((2, nz)),
            dma((2, nz)), dma((2, nz)), dma((2, nz)), dma((2, nz)),
            dma((2, ntp)), dma((2, ntp)),
        ],
        compiler_params=pltpu.CompilerParams(
            collective_id=0, has_side_effects=True, vmem_limit_bytes=VMEM_LIMIT
        ),
    )(
        model_input, value_cotan, mixer_cotan, head_output,
        jnp.stack([value_factor, output_factor]).reshape(2, 2, R // 2, K),
        value_weight, output_weight,
        value_first, output_first, value_second, output_second,
    )


def solution(mesh):
    rows, both, full = P("fs", None), P("fs", "tp"), P(None, "tp")
    return jax.shard_map(
        functools.partial(local, mesh.shape["fs"], mesh.shape["tp"]),
        mesh=mesh,
        in_specs=(rows, both, rows, both) + (both, rows, both, both) * 2,
        out_specs=(both, both, both, both, full) * 2,
        check_vma=False,
    )
```

```python
import functools

import jax
import jax.numpy as jnp
from jax import lax
from jax.experimental import pallas as pl
from jax.experimental.pallas import tpu as pltpu
from jax.sharding import PartitionSpec as P

beta_first = 0.8
beta_second = 0.9
step_rate = 0.02
scale_floor = 0.25
tiny_eps = 1e-08

MESH = pl.DeviceIdType.MESH
F32 = jnp.float32
BF16 = jnp.bfloat16
VMEM_LIMIT = 67_000_000
PLAN = (((1, 0), (1, 1), (1, 3), (1, 2)), ((2, 3),), (), ((2, 2),), (), (), ((2, 1),))


def kernel(
    n,
    ntp,
    rows_v, cols_v, rows_o, cols_o,
    fac_v, fac_o, w_v, w_o, first_v, first_o, second_v, second_o,
    step_v, upd_v, fnew_v, snew_v, copy_v,
    step_o, upd_o, fnew_o, snew_o, copy_o,
    rows, cols, fg, wg, acc, e_buf, pf, pg, send_a, recv_a, send_b, recv_b,
    dirg, ss, ssg,
    sem_rows, sem_cols, sem_fac,
    fs_z, fr_z, fs_y, fr_y, fs_x, fr_x, fs_c, fr_c,
    ws_z, wr_z, ws_y, wr_y,
    as_, ar, bs, br,
    ds_z, dr_z, ds_y, dr_y,
    ps, pr,
):
    nz = n // 2
    me = lax.axis_index("fs")
    tp = lax.axis_index("tp")
    z, y = me // 2, lax.rem(me, 2)
    ybar = 1 - y
    mate = 2 * z + ybar
    core = lax.rem(tp, 2)
    other = 1 - core
    twin = tp + 1 - 2 * core
    half = tp // 2
    far = 1 - half
    across = tp + 2 - 4 * half
    T, D = rows_v.shape
    C = cols_v.shape[1]
    R, K = fac_v.shape[1] * 2, fac_v.shape[2]
    k = first_v.shape[0]
    TC = 512

    def zup(d):
        return lax.rem(z + d, nz)

    def zdn(d):
        return lax.rem(z + nz - d, nz)

    def rcopy(src, dst, ssem, rsem, dev):
        return pltpu.make_async_remote_copy(
            src_ref=src, dst_ref=dst, send_sem=ssem, recv_sem=rsem,
            device_id=dev, device_id_type=MESH,
        )

    def fsdev(i):
        return (i, tp)

    loads = []
    for m, (r, c) in enumerate(((rows_v, cols_v), (rows_o, cols_o))):
        loads.append(pltpu.make_async_copy(r, rows.at[m], sem_rows.at[m]))
        loads.append(pltpu.make_async_copy(c, cols.at[m], sem_cols.at[m]))
    own = [
        pltpu.make_async_copy(r, fg.at[m, me], sem_fac.at[m])
        for m, r in enumerate((fac_v, fac_o))
    ]
    for c in own:
        c.start()
    for i in (0, 2, 1, 3):
        loads[i].start()

    barrier = pltpu.get_barrier_semaphore()
    for d in range(1, nz):
        pl.semaphore_signal(
            barrier, inc=1, device_id=fsdev(2 * zup(d) + y), device_id_type=MESH
        )
    pl.semaphore_signal(barrier, inc=1, device_id=fsdev(mate), device_id_type=MESH)
    for q in range(1, ntp):
        pl.semaphore_signal(
            barrier, inc=1, device_id=(me, lax.rem(tp + q, ntp)), device_id_type=MESH
        )
    pl.semaphore_wait(barrier, nz - 1 + 1 + ntp - 1)

    pend = []
    for c in own:
        c.wait()

    for d in list(range(1, nz)):
        c = rcopy(fg.at[core, me, half], fg.at[core, me, half], fs_z.at[d], fr_z.at[d], fsdev(2 * zup(d) + y))
        c.start()
        pend.append(c)
    c = rcopy(fg.at[core, me, half], fg.at[core, me, half], fs_y.at[0], fr_y.at[0], fsdev(mate))
    c.start()
    pend.append(c)
    wg[me, 0] = w_v[...].astype(BF16)
    wg[me, 1] = w_o[...].astype(BF16)

    def w_send(d):
        if d == 0:
            c = rcopy(wg.at[me], wg.at[me], ws_y.at[0], wr_y.at[0], fsdev(mate))
        else:
            c = rcopy(wg.at[me], wg.at[me], ws_z.at[d], wr_z.at[d], fsdev(2 * zup(d) + y))
        c.start()
        pend.append(c)

    def w_forward(d):
        i = 2 * zdn(d) + y
        rcopy(wg.at[i], wg.at[i], ws_z.at[d], wr_z.at[d], fsdev(mate)).wait_recv()
        c = rcopy(wg.at[i], wg.at[i], ws_y.at[d], wr_y.at[d], fsdev(mate))
        c.start()
        pend.append(c)

    def w_finish(d):
        i = 2 * zdn(d) + ybar
        rcopy(wg.at[i], wg.at[i], ws_y.at[d], wr_y.at[d], fsdev(mate)).wait_recv()

    def act(point):
        for kind, d in PLAN[point]:
            if d < nz:
                (w_send if kind == 1 else w_forward)(d)
        for d in range(4, nz):
            if point == 0:
                w_send(d)
            if point == 5:
                w_forward(d)

    def mine(i):
        return fg.at[core, i, half]

    def to_mates(i, q):
        for src, ssem, rsem, dev in (
            (mine(i), fs_x.at[q], fr_x.at[q], (me, across)),
            (mine(i), fs_c.at[0, q], fr_c.at[0, q], (me, twin)),
        ):
            c = rcopy(src, src, ssem, rsem, dev)
            c.start()
            pend.append(c)

    def f_recv(sems, d, i):
        rcopy(mine(i), mine(i), fs_z.at[0], sems.at[d], fsdev(mate)).wait_recv()

    def f_recv_across(i, q):
        r = fg.at[core, i, far]
        rcopy(r, r, fs_x.at[q], fr_x.at[q], (me, across)).wait_recv()
        c = rcopy(r, r, fs_c.at[1, q], fr_c.at[1, q], (me, twin))
        c.start()
        pend.append(c)

    def f_recv_twin(i, q):
        for g, h in ((0, half), (1, far)):
            r = fg.at[other, i, h]
            rcopy(r, r, fs_c.at[g, q], fr_c.at[g, q], (me, twin)).wait_recv()

    def accumulate(m, d):
        p = zdn(d)
        pair_t = fg[m, pl.ds(2 * p, 2)].reshape(2 * R, K).T

        @pl.loop(0, T // TC)
        def _(t):
            at = pl.ds(pl.multiple_of(t * TC, TC), TC)
            lhs = rows[m, at, pl.ds(pl.multiple_of(p * 2 * R, 2 * R), 2 * R)]
            prod = lax.dot_general(
                pair_t, lhs, (((1,), (1,)), ((), ())), preferred_element_type=F32
            )
            if d == 0:
                acc[m, :, at] = prod
            else:
                acc[m, :, at] += prod

    def arrive(d):
        if d > 0:
            i = 2 * zdn(d) + y
            f_recv(fr_z, d, i)
            c = rcopy(mine(i), mine(i), fs_y.at[d], fr_y.at[d], fsdev(mate))
            c.start()
            pend.append(c)
            to_mates(i, 2 * d)
        i = 2 * zdn(d) + ybar
        f_recv(fr_y, d, i)
        to_mates(i, 2 * d + 1)

    def complete(d):
        qs = ([(2 * zdn(d) + y, 2 * d)] if d else []) + [(2 * zdn(d) + ybar, 2 * d + 1)]
        for i, q in qs:
            f_recv_across(i, q)
        if d == 0:
            loads[0].wait()
            loads[2].wait()
        accumulate(core, d)
        for i, q in qs:
            f_recv_twin(i, q)
        accumulate(other, d)

    for d in range(nz):
        arrive(d)
        if d == 0:
            act(0)
        else:
            complete(d - 1)
    act(6)
    complete(nz - 1)
    loads[1].wait()
    loads[3].wait()

    def partial_products(m):
        @pl.loop(0, T // TC)
        def _(t):
            at = pl.ds(pl.multiple_of(t * TC, TC), TC)
            red = acc[m, :, at].astype(BF16)
            prod = jnp.dot(red, cols[m, at, :], preferred_element_type=F32)
            prod = prod.reshape(n, k, C)

            @pl.when(t == 0)
            def _():
                pf[m] = prod

            @pl.when(t > 0)
            def _():
                pf[m] += prod

        for h in range(nz):
            send_a[m, h] = pf[m, 2 * zup(h) + ybar].astype(BF16)
        for h in [*range(1, nz), 0]:
            c = rcopy(
                send_a.at[m, h], recv_a.at[m, h], as_.at[m, h], ar.at[m, h], fsdev(mate)
            )
            c.start()
            pend.append(c)

    def middle(m):
        for h in [*range(1, nz), 0]:
            rcopy(
                send_a.at[m, h], recv_a.at[m, h], as_.at[m, h], ar.at[m, h], fsdev(mate)
            ).wait_recv()
            tot = pf[m, 2 * zup(h) + y] + recv_a[m, h].astype(F32)
            if h == 0:
                pg[m] = tot
            else:
                send_b[m, h] = tot.astype(BF16)
                c = rcopy(
                    send_b.at[m, h], recv_b.at[m, h], bs.at[m, h], br.at[m, h],
                    fsdev(2 * zup(h) + y),
                )
                c.start()
                pend.append(c)

    def moments(m, first, second, fnew, snew):
        tot = pg[m]
        for h in range(1, nz):
            rcopy(
                send_b.at[m, h], recv_b.at[m, h], bs.at[m, h], br.at[m, h], fsdev(mate)
            ).wait_recv()
            tot = tot + recv_b[m, h].astype(F32)
        f = beta_first * first[...] + (1.0 - beta_first) * tot
        s = beta_second * second[...] + (1.0 - beta_second) * tot * tot
        fnew[...] = f
        snew[...] = s
        dirg[m, me] = (f / (jnp.sqrt(s) + tiny_eps)).astype(BF16)
        for h in range(1, nz):
            c = rcopy(
                dirg.at[m, me], dirg.at[m, me], ds_z.at[m, h], dr_z.at[m, h],
                fsdev(2 * zup(h) + y),
            )
            c.start()
            pend.append(c)
        c = rcopy(dirg.at[m, me], dirg.at[m, me], ds_y.at[m, 0], dr_y.at[m, 0], fsdev(mate))
        c.start()
        pend.append(c)

    def dir_forward(m):
        for h in range(1, nz):
            i = 2 * zdn(h) + y
            rcopy(
                dirg.at[m, i], dirg.at[m, i], ds_z.at[m, h], dr_z.at[m, h], fsdev(mate)
            ).wait_recv()
            c = rcopy(dirg.at[m, i], dirg.at[m, i], ds_y.at[m, h], dr_y.at[m, h], fsdev(mate))
            c.start()
            pend.append(c)

    def expand(m):
        for h in range(nz):
            i = 2 * zdn(h) + ybar
            rcopy(
                dirg.at[m, i], dirg.at[m, i], ds_y.at[m, h], dr_y.at[m, h], fsdev(mate)
            ).wait_recv()
        ss[m] = jnp.zeros(ss.shape[1:], F32)

        @pl.loop(0, nz)
        def _(b):
            lhs = fg[m, pl.ds(2 * b, 2)].reshape(2 * R, K)
            ex = jnp.dot(lhs, dirg[m].reshape(n * k, C), preferred_element_type=F32)
            e_buf[m, pl.ds(2 * b, 2)] = ex.reshape(2, R, C)
            ss[m] += jnp.sum((ex * ex).reshape(2 * R // 8, 8, C), axis=0)

        for q in range(1, ntp):
            c = rcopy(
                ss.at[m], ssg.at[m, q], ps.at[m, q], pr.at[m, q],
                (me, lax.rem(tp + q, ntp)),
            )
            c.start()
            pend.append(c)

    def finish(m, weight, step, upd, copy):
        tot = ss[m]
        for q in range(1, ntp):
            rcopy(ss.at[m], ssg.at[m, q], ps.at[m, q], pr.at[m, q], (me, twin)).wait_recv()
            tot = tot + ssg[m, q]
        mean = jnp.sum(tot, keepdims=True) / (n * R * C * ntp)
        scale = step_rate / jnp.sqrt(mean + scale_floor)
        s = scale * e_buf[m, me]
        step[...] = s
        upd[...] = weight[...] - s

        @pl.loop(0, n)
        def _(b):
            at = pl.ds(pl.multiple_of(b * R, R), R)
            copy[at, :] = (wg[b, m].astype(F32) - scale * e_buf[m, b]).astype(BF16)

    partial_products(0)
    partial_products(1)
    act(1)
    middle(0)
    middle(1)
    act(2)
    moments(0, first_v, second_v, fnew_v, snew_v)
    moments(1, first_o, second_o, fnew_o, snew_o)
    act(3)
    dir_forward(0)
    dir_forward(1)
    act(4)
    expand(0)
    expand(1)
    act(5)
    for h in range(nz):
        w_finish(h)
    finish(0, w_v, step_v, upd_v, copy_v)
    finish(1, w_o, step_o, upd_o, copy_o)
    for c in pend:
        c.wait_send()


def deliver(count, *refs):
    srcs, dsts, bufs = refs[:count], refs[count:2 * count], refs[2 * count:3 * count]
    sem_in, sem_out = refs[3 * count:]
    ins = [pltpu.make_async_copy(a, b, sem_in.at[i]) for i, (a, b) in enumerate(zip(srcs, bufs))]
    outs = [pltpu.make_async_copy(a, b, sem_out.at[i]) for i, (a, b) in enumerate(zip(bufs, dsts))]
    for c in ins:
        c.start()
    for a, b in zip(ins, outs):
        a.wait()
        b.start()
    for c in outs:
        c.wait()


def local(
    n, ntp,
    model_input, value_cotan, mixer_cotan, head_output,
    value_weight, value_factor, value_first, value_second,
    output_weight, output_factor, output_first, output_second,
):
    T, D = model_input.shape
    C = value_cotan.shape[1]
    R, K = value_factor.shape
    k = value_first.shape[0]
    nz = n // 2
    vm = pl.BlockSpec(memory_space=pltpu.VMEM)
    hbm = pl.BlockSpec(memory_space=pl.ANY)
    wide = jax.ShapeDtypeStruct((R, C), F32)
    mom = jax.ShapeDtypeStruct((k, C), F32)
    full = jax.ShapeDtypeStruct((n * R, C), BF16)
    dma = pltpu.SemaphoreType.DMA
    results = pl.pallas_call(
        functools.partial(kernel, n, ntp),
        out_shape=(wide, wide, mom, mom, full) * 2,
        in_specs=[hbm] * 6 + [vm] * 6,
        out_specs=(vm,) * 10,
        scratch_shapes=[
            pltpu.VMEM((2, T, D), BF16),
            pltpu.VMEM((2, T, C), BF16),
            pltpu.VMEM((2, n, 2, R // 2, K), BF16),
            pltpu.VMEM((n, 2, R, C), BF16),
            pltpu.VMEM((2, K, T), F32),
            pltpu.VMEM((2, n, R, C), F32),
            pltpu.VMEM((2, n, k, C), F32),
            pltpu.VMEM((2, k, C), F32),
            pltpu.VMEM((2, nz, k, C), BF16),
            pltpu.VMEM((2, nz, k, C), BF16),
            pltpu.VMEM((2, nz, k, C), BF16),
            pltpu.VMEM((2, nz, k, C), BF16),
            pltpu.VMEM((2, n, k, C), BF16),
            pltpu.VMEM((2, 8, C), F32),
            pltpu.VMEM((2, ntp, 8, C), F32),
            dma((2,)), dma((2,)), dma((2,)),
            dma((nz,)), dma((nz,)), dma((nz,)), dma((nz,)), dma((n,)), dma((n,)), dma((2, n)), dma((2, n)),
            dma((nz,)), dma((nz,)), dma((nz,)), dma((nz,)),
            dma((2, nz)), dma((2, nz)), dma((2, nz)), dma((2, nz)),
            dma((2, nz)), dma((2, nz)), dma((2, nz)), dma((2, nz)),
            dma((2, ntp)), dma((2, ntp)),
        ],
        compiler_params=pltpu.CompilerParams(
            collective_id=0, has_side_effects=True, vmem_limit_bytes=VMEM_LIMIT
        ),
    )(
        model_input, value_cotan, mixer_cotan, head_output,
        value_factor.reshape(2, R // 2, K), output_factor.reshape(2, R // 2, K),
        value_weight, output_weight,
        value_first, output_first, value_second, output_second,
    )
    return pl.pallas_call(
        functools.partial(deliver, len(results)),
        out_shape=tuple(jax.ShapeDtypeStruct(r.shape, r.dtype) for r in results),
        in_specs=[hbm] * len(results),
        out_specs=(hbm,) * len(results),
        scratch_shapes=[pltpu.VMEM(r.shape, r.dtype) for r in results]
        + [dma((len(results),)), dma((len(results),))],
    )(*results)


def solution(mesh):
    rows, both, full = P("fs", None), P("fs", "tp"), P(None, "tp")
    return jax.shard_map(
        functools.partial(local, mesh.shape["fs"], mesh.shape["tp"]),
        mesh=mesh,
        in_specs=(rows, both, rows, both) + (both, rows, both, both) * 2,
        out_specs=(both, both, both, both, full) * 2,
        check_vma=False,
    )
```
